512 devices in a mesh: grp: 2 (over y), sp: 32 (over z, core), tp: 8 (over x).
Axes of the slice: x: 8, y: 2, z: 16, core: 2. Of those that a mesh axis runs over, the one named last changes fastest.
The devices are a block of a 8x8x16 slice.
Arguments:
- prompt_rows: bfloat16 [49152, 2048], P(('grp', 'sp')), parts along dimension 0, may hold values from -6 to 6
- norm_gain: float32 [2048], replicated, may hold values from 0.1 to 1.9
- key_weight: bfloat16 [2048, 1024], P(None, 'tp'), may hold values from -0.125 to 0.125
- value_weight: bfloat16 [2048, 1024], P(None, 'tp'), may hold values from -0.125 to 0.125
- new_query: bfloat16 [2048], P(('grp', 'tp')), parts along dimension 0, may hold values from -6 to 6
- score_offset: float32 [16], P('tp'), may hold values from -11.5 to -4
- output_gain: float32 [1024], P('tp'), may hold values from 0.1 to 1.9
Outputs:
- key_cache: bfloat16 [16, 32, 32, 48, 64], P(('grp', 'tp'), 'sp'), parts along dimension 0
- value_cache: bfloat16 [16, 32, 32, 48, 64], P(('grp', 'tp'), 'sp'), parts along dimension 0
- first_read: bfloat16 [2048], P(('grp', 'tp')), parts along dimension 0
The draws below stay inside these ranges and needn't reach their ends.
There are 2 independent parts, one for each index of `grp`. The reference program is written for one: setup_inputs(seed, part) draws one part's arguments, and reference() takes and returns one part's arrays. A program takes and returns all parts, laid end to end along the dimension named above; an argument that names none is the same for every part. Nothing has to cross between parts.
All inputs are finite; a program needn't handle non-finite values.
Results may differ from the reference program's by a relative error of at most 0.0059.
Values may be sent and summed in bfloat16 or wider, within the bound.
No kernel may reach another device: no remote copies, remote signals or barrier semaphores. Data moves between devices by JAX's collectives and lax.ppermute only.
A program may use at most 64 MiB of HBM per device.

```python
import jax
import jax.numpy as jnp
from jax import lax

WIDTH = 2048
HEADS = 16
HEAD_DIM = 64
LEN = 24576
HEADS_DEV = 2
SUBS = 16
ROWS = 48
N_SP = 32
N_TP = 8


def steps_of(stream_key, extent, cuts, least, top_value):
    gain, own = 1.0, jax.random.fold_in(stream_key, 6)
    for position, parts in cuts:
        heights = jnp.exp(jax.random.uniform(jax.random.fold_in(own, position), (parts,), jnp.float32, least / len(cuts), top_value / len(cuts)))
        gain = gain * jnp.repeat(heights, extent[position] // parts).reshape([-1 if axis == position else 1 for axis in range(len(extent))])
    return gain


def normal_values(key, extent, scale, most, cuts=(), dtype=jnp.bfloat16):
    level = steps_of(key, extent, cuts, -0.22, 0.18) if cuts else 1.0
    values = jax.random.normal(key, extent, jnp.float32) * scale * level
    return jnp.minimum(jnp.maximum(values, -most), most).astype(dtype)


def setup_inputs(seed: int = 0, part: int = 0) -> dict:
    key_of = jax.random.split(jax.random.key(seed), 8)
    part_splits = jax.random.split(jax.random.fold_in(key_of[7], part), 8)
    return {
        "prompt_rows": normal_values(part_splits[0], (LEN, WIDTH), 1.0, 6.0, ((0, 32),)),
        "norm_gain": jnp.clip(1.0 + 0.18 * jax.random.normal(key_of[1], (WIDTH,), jnp.float32), 0.1, 1.9),
        "key_weight": normal_values(key_of[2], (WIDTH, HEADS * HEAD_DIM), WIDTH ** -0.5, 0.125, ((1, 8),)),
        "value_weight": normal_values(key_of[3], (WIDTH, HEADS * HEAD_DIM), WIDTH ** -0.5, 0.125, ((1, 8),)),
        "new_query": normal_values(part_splits[4], (HEADS * HEAD_DIM,), 1.0, 6.0, ((0, 8),)),
        "score_offset": jnp.clip(-11.5 + 7.5 * jax.random.uniform(key_of[5], (HEADS,), jnp.float32) ** steps_of(key_of[5], (HEADS,), ((0, 8),), -0.2, 0.2), -11.5, -4.0),
        "output_gain": jnp.clip(1.0 + 0.18 * jax.random.normal(key_of[6], (HEADS * HEAD_DIM,), jnp.float32), 0.1, 1.9),
    }


EPSILON = 1e-06

def layout(cache):
    split = cache.reshape(N_SP, SUBS, ROWS, N_TP, HEADS_DEV, HEAD_DIM)
    moved = jnp.transpose(split, (3, 4, 1, 0, 2, 5))
    return moved.reshape(N_TP, N_SP, N_SP, ROWS, HEAD_DIM)

def reference(prompt_rows, norm_gain, key_weight, value_weight, new_query, score_offset, output_gain):
    rows32 = prompt_rows.astype(jnp.float32)
    mean_square = lax.optimization_barrier(jnp.mean(rows32 * rows32, axis=-1, keepdims=True))
    normed = (rows32 * lax.rsqrt(mean_square + EPSILON) * norm_gain).astype(jnp.bfloat16)
    keys = jnp.dot(normed, key_weight, preferred_element_type=jnp.float32).astype(jnp.bfloat16)
    values = jnp.dot(normed, value_weight, preferred_element_type=jnp.float32).astype(jnp.bfloat16)
    keys3 = keys.reshape(LEN, HEADS, HEAD_DIM).astype(jnp.float32)
    values3 = values.reshape(LEN, HEADS, HEAD_DIM).astype(jnp.float32)
    query2 = new_query.reshape(HEADS, HEAD_DIM).astype(jnp.float32)
    scores = jnp.einsum('hd,shd->hs', query2, keys3) * HEAD_DIM ** (-0.5) + score_offset[:, None]
    remain = jax.nn.log_sigmoid(-scores)
    after_sum = lax.cumsum(remain, axis=1, reverse=True) - remain
    sticks = jnp.exp(jax.nn.log_sigmoid(scores) + after_sum).astype(jnp.bfloat16)
    sticks32 = lax.optimization_barrier(sticks).astype(jnp.float32)
    mixed = jnp.einsum('hs,shd->hd', sticks32, values3)
    spread = lax.optimization_barrier(jnp.mean(mixed * mixed, axis=-1, keepdims=True))
    result = mixed * lax.rsqrt(spread + EPSILON) * output_gain.reshape(HEADS, HEAD_DIM)
    return (layout(keys), layout(values), result.reshape(HEADS * HEAD_DIM).astype(jnp.bfloat16))
```

```python
import jax
import jax.numpy as jnp
from jax import lax
from jax.experimental import pallas as pl
from jax.experimental.pallas import tpu as pltpu
from jax.sharding import PartitionSpec as P

EPSILON = 1e-06
HIGHEST = lax.Precision.HIGHEST
EXTRA = 8
STEPS = 4


def split3(value):
    high = value.astype(jnp.bfloat16).astype(jnp.float32)
    rest = value - high
    middle = rest.astype(jnp.bfloat16).astype(jnp.float32)
    return high, middle, rest - middle


def fill_kernel(
    x_hbm, gain_ref, kw_hbm, vw_hbm, query_ref, offset_ref, out_ref, x_ref, w_ref, x_sem, w_sem
):
    steps, tile, _ = x_ref.shape
    columns = kw_hbm.shape[1]
    half = columns // 2
    rows = out_ref.shape[3] - EXTRA
    pairs = tile // rows // 2

    key_copy = pltpu.make_async_copy(kw_hbm, w_ref.at[:, pl.ds(0, columns)], w_sem.at[0])
    value_copy = pltpu.make_async_copy(vw_hbm, w_ref.at[:, pl.ds(columns, columns)], w_sem.at[1])
    copies = [
        pltpu.make_async_copy(x_hbm.at[pl.ds(i * tile, tile), :], x_ref.at[i], x_sem.at[i])
        for i in range(steps)
    ]
    copies[steps - 1].start()
    key_copy.start()
    value_copy.start()
    for i in reversed(range(steps - 1)):
        copies[i].start()

    low = lax.broadcasted_iota(jnp.int32, (tile, columns), 1) < half
    low8 = lax.broadcasted_iota(jnp.int32, (8, columns), 1) < half
    query = query_ref[...].astype(jnp.float32)
    queries = [
        jnp.where(low8, query, 0.0).astype(jnp.bfloat16),
        jnp.where(low8, pltpu.roll(query, half, 1), 0.0).astype(jnp.bfloat16),
    ]
    upper = (
        lax.broadcasted_iota(jnp.int32, (tile, tile), 0)
        > lax.broadcasted_iota(jnp.int32, (tile, tile), 1)
    ).astype(jnp.float32)
    later = [jnp.zeros((8, 1), jnp.float32) for _ in range(2)]
    mixed = [jnp.zeros((8, columns), jnp.float32) for _ in range(2)]
    for i in reversed(range(steps)):
        copies[i].wait()
        x32 = x_ref[i].astype(jnp.float32)
        mean_square = jnp.mean(x32 * x32, axis=-1, keepdims=True)
        normed = (x32 * lax.rsqrt(mean_square + EPSILON) * gain_ref[...]).astype(jnp.bfloat16)
        if i == steps - 1:
            key_copy.wait()
            value_copy.wait()
        both = jnp.dot(normed, w_ref[...], preferred_element_type=jnp.float32)
        keys, values = both[:, :columns], both[:, columns:]
        heads = [
            jnp.where(low, keys, pltpu.roll(values, half, 1)).astype(jnp.bfloat16),
            jnp.where(low, pltpu.roll(keys, half, 1), values).astype(jnp.bfloat16),
        ]
        for h in range(2):
            head = heads[h]
            for j in range(2 * pairs):
                out_ref[j % 2, h, i * pairs + j // 2, 0:rows, :] = head[j * rows : (j + 1) * rows]
            scores = lax.dot_general(
                queries[h], head, (((1,), (1,)), ((), ())), preferred_element_type=jnp.float32
            )
            scores = scores * half ** (-0.5) + offset_ref[h]
            soft = jnp.log1p(jnp.exp(-jnp.abs(scores)))
            remain = -(jnp.maximum(scores, 0.0) + soft)
            taken = jnp.minimum(scores, 0.0) - soft
            within = jnp.dot(remain, upper, precision=HIGHEST, preferred_element_type=jnp.float32)
            sticks = jnp.exp(taken + within + later[h])
            rounded = sticks.astype(jnp.bfloat16)
            rest = (sticks - rounded.astype(jnp.float32)).astype(jnp.bfloat16)
            mixed[h] = mixed[h] + jnp.dot(rounded, head, preferred_element_type=jnp.float32)
            mixed[h] = mixed[h] + jnp.dot(rest, head, preferred_element_type=jnp.float32)
            later[h] = later[h] + jnp.sum(remain, axis=1, keepdims=True)

    line = lax.broadcasted_iota(jnp.int32, (8, columns), 0)
    lane = lax.broadcasted_iota(jnp.int32, (8, columns), 1)
    weighted = jnp.where(low8, pltpu.roll(mixed[0], half, 1), mixed[1])
    high = weighted.astype(jnp.bfloat16).astype(jnp.float32)
    sums = jnp.zeros((8, columns), jnp.float32)
    for at, part in enumerate(split3(later[0]) + split3(later[1])):
        sums = jnp.where(lane == at, part, sums)
    payload = jnp.where(line == 0, high, jnp.where(line == 1, weighted - high, 0.0))
    payload = jnp.where(line == 2, sums, payload).astype(jnp.bfloat16)
    shape = (*out_ref.shape[:3], EXTRA, columns)
    out_ref[:, :, :, rows:, :] = jnp.broadcast_to(payload, shape)


def fill(rows, norm_gain, key_weight, value_weight, query, offset, subs):
    count, width = rows.shape
    columns = key_weight.shape[1]
    sub_rows = count // subs
    heads = offset.shape[0]
    tile = count // STEPS
    vmem = pl.BlockSpec(memory_space=pltpu.VMEM)
    hbm = pl.BlockSpec(memory_space=pl.ANY)
    return pl.pallas_call(
        fill_kernel,
        in_specs=[hbm, vmem, hbm, hbm, vmem, pl.BlockSpec(memory_space=pltpu.SMEM)],
        out_specs=vmem,
        out_shape=jax.ShapeDtypeStruct((2, heads, subs // 2, sub_rows + EXTRA, columns), jnp.bfloat16),
        scratch_shapes=[
            pltpu.VMEM((STEPS, tile, width), jnp.bfloat16),
            pltpu.VMEM((width, 2 * columns), jnp.bfloat16),
            pltpu.SemaphoreType.DMA((STEPS,)),
            pltpu.SemaphoreType.DMA((2,)),
        ],
        name="fill",
    )(rows, norm_gain.reshape(1, width), key_weight, value_weight, query, offset)


def settle_kernel(moved_ref, gain_ref, keys_ref, values_ref, read_ref):
    peers, rows, half = moved_ref.shape[0], keys_ref.shape[2], keys_ref.shape[3]
    columns = 2 * half
    chips = peers // 2
    for c in range(2):
        both = moved_ref[c * chips : (c + 1) * chips, 0:rows, :]
        keys_ref[:, c] = both[:, :, :half]
        values_ref[:, c] = both[:, :, half:]

    payload = moved_ref[:, rows:, :].astype(jnp.float32)
    line = lax.broadcasted_iota(jnp.int32, payload.shape, 1)
    weighted = jnp.sum(jnp.where(line < 2, payload, 0.0), axis=1)
    sums = jnp.sum(jnp.where(line == 2, payload, 0.0), axis=1)
    at_row = lax.broadcasted_iota(jnp.int32, (peers, peers), 0)
    at_col = lax.broadcasted_iota(jnp.int32, (peers, peers), 1)
    block_row = lax.rem(at_row, chips) * 2 + at_row // chips
    block_col = lax.rem(at_col, chips) * 2 + at_col // chips
    after = (block_col > block_row).astype(jnp.float32)
    beyond = jnp.dot(after, sums, precision=HIGHEST, preferred_element_type=jnp.float32)
    lane = lax.broadcasted_iota(jnp.int32, (peers, columns), 1)
    first = jnp.sum(jnp.where(lane < 3, beyond, 0.0), axis=1, keepdims=True)
    second = jnp.sum(jnp.where((lane >= 3) & (lane < 6), beyond, 0.0), axis=1, keepdims=True)
    low = lane < half
    mixed = jnp.sum(weighted * jnp.exp(jnp.where(low, first, second)), axis=0, keepdims=True)
    low = low[0:1]
    square = mixed * mixed
    first = jnp.sum(jnp.where(low, square, 0.0), axis=1, keepdims=True) / half
    second = jnp.sum(jnp.where(low, 0.0, square), axis=1, keepdims=True) / half
    scale = lax.rsqrt(jnp.where(low, first, second) + EPSILON)
    read_ref[...] = (mixed * scale * gain_ref[...]).astype(jnp.bfloat16)


def settle(moved, gain):
    peers, rows, columns = moved.shape
    rows = rows - EXTRA
    cache = jax.ShapeDtypeStruct((peers // 2, 2, rows, columns // 2), jnp.bfloat16)
    vmem = pl.BlockSpec(memory_space=pltpu.VMEM)
    return pl.pallas_call(
        settle_kernel,
        in_specs=[vmem, vmem],
        out_specs=[vmem, vmem, vmem],
        out_shape=[cache, cache, jax.ShapeDtypeStruct((1, columns), jnp.bfloat16)],
        name="settle",
    )(moved, gain.reshape(1, columns))


def body(prompt_rows, norm_gain, key_weight, value_weight, new_query, score_offset, output_gain):
    heads = score_offset.shape[0]
    peers = lax.axis_size("sp")
    subs = peers // heads
    columns = key_weight.shape[1]
    query = jnp.broadcast_to(new_query.reshape(1, columns), (8, columns))
    packed = fill(prompt_rows, norm_gain, key_weight, value_weight, query, score_offset, subs)
    block = packed.shape[3]
    order = [*range(0, peers, 2), *range(1, peers, 2)]
    moved = lax.all_to_all(
        packed.reshape(peers, block, columns), "sp", 0, 0, axis_index_groups=[order], tiled=True
    )
    keys, values, first_read = settle(moved, output_gain)
    target = (1, 1, peers, block - EXTRA, columns // heads)
    return (keys.reshape(target), values.reshape(target), first_read.reshape(columns))


def solution(mesh):
    in_specs = (
        P(("grp", "sp"), None),
        P(),
        P(None, "tp"),
        P(None, "tp"),
        P(("grp", "tp")),
        P("tp"),
        P("tp"),
    )
    out_specs = (
        P(("grp", "tp"), "sp", None, None, None),
        P(("grp", "tp"), "sp", None, None, None),
        P(("grp", "tp")),
    )
    return jax.shard_map(body, mesh=mesh, in_specs=in_specs, out_specs=out_specs, check_vma=False)
```

```python
import jax
import jax.numpy as jnp
from jax import lax
from jax.experimental import pallas as pl
from jax.experimental.pallas import tpu as pltpu
from jax.sharding import PartitionSpec as P

EPSILON = 1e-06
STEPS = 2
APART = 4
GROUP = 32


def split3(value):
    high = value.astype(jnp.bfloat16).astype(jnp.float32)
    rest = value - high
    middle = rest.astype(jnp.bfloat16).astype(jnp.float32)
    return high, middle, rest - middle


def fill_kernel(
    x_hbm, gain_hbm, kw_hbm, vw_hbm, query_hbm, offset_hbm, out_ref,
    x_ref, w_ref, gain_ref, query_ref, offset_ref, normed_ref, head_ref, x_sem, w_sem, sem,
):
    steps, tile, _ = x_ref.shape
    columns = kw_hbm.shape[1]
    half = columns // 2
    rows = 2 * (out_ref.shape[3] - 1)
    apart, chips = out_ref.shape[1], out_ref.shape[1] * out_ref.shape[2]
    count = steps * tile
    chunks = count // columns

    copies = [
        pltpu.make_async_copy(x_hbm.at[pl.ds(i * tile, tile), :], x_ref.at[i], x_sem.at[i])
        for i in range(steps)
    ]
    gain_copy = pltpu.make_async_copy(gain_hbm, gain_ref, sem.at[0])
    query_copy = pltpu.make_async_copy(query_hbm, query_ref, sem.at[1])
    offset_copy = pltpu.make_async_copy(offset_hbm, offset_ref, sem.at[2])
    key_copy = pltpu.make_async_copy(kw_hbm, w_ref.at[:, pl.ds(0, columns)], w_sem.at[0])
    value_copy = pltpu.make_async_copy(vw_hbm, w_ref.at[:, pl.ds(columns, columns)], w_sem.at[1])
    gain_copy.start()
    key_copy.start()
    value_copy.start()
    copies[0].start()
    for i in range(1, steps):
        copies[i].start(priority=1)
    query_copy.start()
    offset_copy.start()

    low = lax.broadcasted_iota(jnp.int32, (tile, columns), 1) < half

    pairs = tile // rows // 2

    def multiply(i, carry):
        pltpu.make_async_copy(
            x_hbm.at[pl.ds(i * tile, tile), :], x_ref.at[i], x_sem.at[i]
        ).wait()
        for r in range(0, tile, GROUP):
            x32 = x_ref[i, r : r + GROUP, :].astype(jnp.float32)
            mean_square = jnp.mean(x32 * x32, axis=-1, keepdims=True)
            scale = lax.rsqrt(mean_square + EPSILON)
            normed_ref[r : r + GROUP, :] = (x32 * scale * gain_ref[...]).astype(jnp.bfloat16)
        both = jnp.dot(normed_ref[...], w_ref[...], preferred_element_type=jnp.float32)
        keys, values = both[:, :columns], both[:, columns:]
        heads = [
            jnp.where(low, keys, pltpu.roll(values, half, 1)).astype(jnp.bfloat16),
            jnp.where(low, pltpu.roll(keys, half, 1), values).astype(jnp.bfloat16),
        ]
        for h in range(2):
            head_ref[h, pl.ds(i * tile, tile), :] = heads[h]
            for j in range(2 * pairs):
                chip = h * (chips // 2) + i * pairs + j // 2
                out_ref[j % 2, lax.rem(chip, apart), lax.div(chip, apart), 0 : rows // 2] = heads[h][
                    j * rows : (j + 1) * rows
                ].reshape(rows // 2, 2, columns)
        return carry

    gain_copy.wait()
    key_copy.wait()
    value_copy.wait()
    lax.fori_loop(0, steps, multiply, 0)
    query_copy.wait()
    offset_copy.wait()

    low8 = lax.broadcasted_iota(jnp.int32, (8, columns), 1) < half
    query = jnp.broadcast_to(query_ref[...].astype(jnp.float32), (8, columns))
    queries = [
        jnp.where(low8, query, 0.0).astype(jnp.bfloat16),
        jnp.where(low8, pltpu.roll(query, half, 1), 0.0).astype(jnp.bfloat16),
    ]
    upper = (
        lax.broadcasted_iota(jnp.int32, (columns, columns), 0)
        > lax.broadcasted_iota(jnp.int32, (columns, columns), 1)
    ).astype(jnp.bfloat16)
    scores = jnp.concatenate(
        [
            lax.dot_general(
                queries[h], head_ref[h], (((1,), (1,)), ((), ())), preferred_element_type=jnp.float32
            )
            * half ** (-0.5)
            + offset_ref[h]
            for h in range(2)
        ],
        axis=0,
    )
    soft = jnp.log1p(jnp.exp(-jnp.abs(scores)))
    remain = -(jnp.maximum(scores, 0.0) + soft)
    taken = jnp.minimum(scores, 0.0) - soft
    pieces = [remain[:, c * columns : (c + 1) * columns] for c in range(chunks)]
    stacked = jnp.concatenate(
        [part.astype(jnp.bfloat16) for piece in pieces for part in split3(piece)], axis=0
    )
    summed = jnp.dot(stacked, upper, preferred_element_type=jnp.float32)
    later = jnp.zeros((16, 1), jnp.float32)
    after = [None] * chunks
    for c in reversed(range(chunks)):
        base = c * 48
        within = summed[base : base + 16] + summed[base + 16 : base + 32] + summed[base + 32 : base + 48]
        after[c] = within + later
        later = later + jnp.sum(pieces[c], axis=1, keepdims=True)
    sticks = jnp.exp(taken + jnp.concatenate(after, axis=1))
    rounded = sticks.astype(jnp.bfloat16).astype(jnp.float32)
    rest = sticks - rounded
    mixed = []
    for h in range(2):
        parts = jnp.concatenate([rounded[h * 8 : h * 8 + 8], rest[h * 8 : h * 8 + 8]], axis=0)
        products = jnp.dot(
            parts.astype(jnp.bfloat16), head_ref[h], preferred_element_type=jnp.float32
        )
        mixed.append(products[0:8] + products[8:16])

    line = lax.broadcasted_iota(jnp.int32, (8, columns), 0)
    lane = lax.broadcasted_iota(jnp.int32, (8, columns), 1)
    weighted = jnp.where(low8, pltpu.roll(mixed[0], half, 1), mixed[1])
    sums = jnp.zeros((8, columns), jnp.float32)
    for at, part in enumerate(split3(later[0:8]) + split3(later[8:16])):
        sums = jnp.where(lane == at, part, sums)
    payload = jnp.where(line == 0, weighted, sums)[0:2].astype(jnp.bfloat16)
    shape = (*out_ref.shape[:3], 1, 2, columns)
    out_ref[:, :, :, rows // 2 :] = jnp.broadcast_to(payload, shape)


def fill(rows, norm_gain, key_weight, value_weight, query, offset, subs):
    count, width = rows.shape
    columns = key_weight.shape[1]
    sub_rows = count // subs
    heads = offset.shape[0]
    tile = count // STEPS
    hbm = pl.BlockSpec(memory_space=pl.ANY)
    chips = heads * subs // 2
    out_shape = (2, APART, chips // APART, sub_rows // 2 + 1, 2, columns)
    return pl.pallas_call(
        fill_kernel,
        in_specs=[hbm] * 6,
        out_specs=pl.BlockSpec(memory_space=pltpu.VMEM),
        out_shape=pltpu.VMEM(out_shape, jnp.bfloat16),
        scratch_shapes=[
            pltpu.VMEM((STEPS, tile, width), jnp.bfloat16),
            pltpu.VMEM((width, 2 * columns), jnp.bfloat16),
            pltpu.VMEM((1, width), jnp.float32),
            pltpu.VMEM((1, columns), jnp.bfloat16),
            pltpu.SMEM((heads,), jnp.float32),
            pltpu.VMEM((tile, width), jnp.bfloat16),
            pltpu.VMEM((heads, count, columns), jnp.bfloat16),
            pltpu.SemaphoreType.DMA((STEPS,)),
            pltpu.SemaphoreType.DMA((2,)),
            pltpu.SemaphoreType.DMA((3,)),
        ],
        name="fill",
    )(
        rows, norm_gain.reshape(1, width), key_weight, value_weight,
        query.reshape(1, columns), offset,
    )


def block_of(at, chips):
    near = chips // APART
    inside = at % chips
    return (inside % near * APART + inside // near) * 2 + at // chips


def settle_kernel(
    moved_ref, gain_ref, keys_hbm, values_hbm, read_hbm, keys_ref, values_ref, read_ref, sem
):
    peers, rows, half = moved_ref.shape[0], keys_ref.shape[3], keys_ref.shape[4]
    columns = 2 * half
    chips = peers // 2
    copies = []
    near = chips // APART
    for c in range(2):
        both = moved_ref[c * chips : (c + 1) * chips, 0 : rows // 2]
        both = both.reshape(chips, rows, columns)
        for i in range(APART):
            keys_ref[c, :, i] = both[i * near : (i + 1) * near, :, :half]
        copies.append(pltpu.make_async_copy(keys_ref.at[c], keys_hbm.at[:, :, c], sem.at[2 * c]))
        copies[-1].start()
        for i in range(APART):
            values_ref[c, :, i] = both[i * near : (i + 1) * near, :, half:]
        copies.append(
            pltpu.make_async_copy(values_ref.at[c], values_hbm.at[:, :, c], sem.at[2 * c + 1])
        )
        copies[-1].start()

    payload = moved_ref[:, rows // 2].astype(jnp.float32)
    weighted, sums = payload[:, 0, :], payload[:, 1, :]
    at_row = lax.broadcasted_iota(jnp.int32, (peers, peers), 0)
    at_col = lax.broadcasted_iota(jnp.int32, (peers, peers), 1)
    after = (block_of(at_col, chips) > block_of(at_row, chips)).astype(jnp.bfloat16)
    beyond = jnp.dot(after, sums.astype(jnp.bfloat16), preferred_element_type=jnp.float32)
    lane = lax.broadcasted_iota(jnp.int32, (peers, columns), 1)
    first = jnp.sum(jnp.where(lane < 3, beyond, 0.0), axis=1, keepdims=True)
    second = jnp.sum(jnp.where((lane >= 3) & (lane < 6), beyond, 0.0), axis=1, keepdims=True)
    low = lane < half
    mixed = jnp.sum(weighted * jnp.exp(jnp.where(low, first, second)), axis=0, keepdims=True)
    low = low[0:1]
    square = mixed * mixed
    first = jnp.sum(jnp.where(low, square, 0.0), axis=1, keepdims=True) / half
    second = jnp.sum(jnp.where(low, 0.0, square), axis=1, keepdims=True) / half
    scale = lax.rsqrt(jnp.where(low, first, second) + EPSILON)
    read_ref[...] = (mixed * scale * gain_ref[...]).astype(jnp.bfloat16)
    copies.append(pltpu.make_async_copy(read_ref, read_hbm, sem.at[4]))
    copies[-1].start()
    for copy in copies:
        copy.wait()


def settle(moved, gain):
    peers, rows, _, columns = moved.shape
    rows, half = 2 * (rows - 1), columns // 2
    chips = (peers // 2 // APART, APART)
    cache = jax.ShapeDtypeStruct((*chips, 2, rows, half), jnp.bfloat16)
    vmem = pl.BlockSpec(memory_space=pltpu.VMEM)
    hbm = pl.BlockSpec(memory_space=pl.ANY)
    buffer = pltpu.VMEM((2, *chips, rows, half), jnp.bfloat16)
    return pl.pallas_call(
        settle_kernel,
        in_specs=[vmem, vmem],
        out_specs=[hbm, hbm, hbm],
        out_shape=[cache, cache, jax.ShapeDtypeStruct((1, columns), jnp.bfloat16)],
        scratch_shapes=[
            buffer, buffer, pltpu.VMEM((1, columns), jnp.bfloat16), pltpu.SemaphoreType.DMA((5,)),
        ],
        name="settle",
    )(
        pltpu.with_memory_space_constraint(moved, pltpu.VMEM),
        pltpu.with_memory_space_constraint(gain.reshape(1, columns), pltpu.VMEM),
    )


def body(prompt_rows, norm_gain, key_weight, value_weight, new_query, score_offset, output_gain):
    heads = score_offset.shape[0]
    peers = lax.axis_size("sp")
    subs = peers // heads
    columns = key_weight.shape[1]
    packed = fill(prompt_rows, norm_gain, key_weight, value_weight, new_query, score_offset, subs)
    packed = packed.reshape(peers, *packed.shape[3:])
    order = [block_of(at, peers // 2) for at in range(peers)]
    moved = lax.all_to_all(
        packed, "sp", split_axis=0, concat_axis=0, axis_index_groups=[order], tiled=True
    )
    keys, values, first_read = settle(moved, output_gain)
    target = (1, 1, peers, 2 * (packed.shape[1] - 1), columns // heads)
    return (keys.reshape(target), values.reshape(target), first_read.reshape(columns))


def solution(mesh):
    in_specs = (
        P(("grp", "sp"), None),
        P(),
        P(None, "tp"),
        P(None, "tp"),
        P(("grp", "tp")),
        P("tp"),
        P("tp"),
    )
    out_specs = (
        P(("grp", "tp"), "sp", None, None, None),
        P(("grp", "tp"), "sp", None, None, None),
        P(("grp", "tp")),
    )
    return jax.shard_map(body, mesh=mesh, in_specs=in_specs, out_specs=out_specs, check_vma=False)
```

```python
import functools

import jax
import jax.numpy as jnp
from jax import lax
from jax.experimental import pallas as pl
from jax.experimental.pallas import tpu as pltpu
from jax.sharding import PartitionSpec as P

EPSILON = 1e-06
STEPS = 2
PARTS = 4
GROUP = 32
ORDER = [2 * (z + 4 * j) + c for c in (1, 0) for z in range(4) for j in range(4)]


def split3(value):
    high = value.astype(jnp.bfloat16).astype(jnp.float32)
    rest = value - high
    middle = rest.astype(jnp.bfloat16).astype(jnp.float32)
    return high, middle, rest - middle


def fill_kernel(
    places, x_hbm, gain_hbm, kw_hbm, vw_hbm, query_hbm, offset_hbm, out_ref,
    x_ref, w_ref, gain_ref, query_ref, offset_ref, normed_ref, head_ref, x_sem, w_sem, sem,
):
    steps, tile, _ = x_ref.shape
    columns = kw_hbm.shape[1]
    half = columns // 2
    rows = 2 * (out_ref.shape[1] - 1)
    count = steps * tile
    chunks = count // columns

    part = tile // PARTS

    def part_copy(i, p):
        return pltpu.make_async_copy(
            x_hbm.at[pl.ds(i * tile + p * part, part), :],
            x_ref.at[i, pl.ds(p * part, part), :],
            x_sem.at[i, p],
        )

    gain_copy = pltpu.make_async_copy(gain_hbm, gain_ref, sem.at[0])
    query_copy = pltpu.make_async_copy(query_hbm, query_ref, sem.at[1])
    offset_copy = pltpu.make_async_copy(offset_hbm, offset_ref, sem.at[2])
    key_copy = pltpu.make_async_copy(kw_hbm, w_ref.at[:, pl.ds(0, columns)], w_sem.at[0])
    value_copy = pltpu.make_async_copy(vw_hbm, w_ref.at[:, pl.ds(columns, columns)], w_sem.at[1])
    gain_copy.start()
    part_copy(0, 0).start()
    key_copy.start()
    value_copy.start()
    for i in range(steps):
        for p in range(PARTS):
            if i + p:
                part_copy(i, p).start(priority=1)
    query_copy.start(priority=1)
    offset_copy.start(priority=1)

    low = lax.broadcasted_iota(jnp.int32, (tile, columns), 1) < half

    tile_subs = tile // rows

    def multiply(i, carry):
        for p in range(PARTS):
            part_copy(i, p).wait()
            for r in range(p * part, (p + 1) * part, GROUP):
                x32 = x_ref[i, r : r + GROUP, :].astype(jnp.float32)
                mean_square = jnp.mean(x32 * x32, axis=-1, keepdims=True)
                scale = lax.rsqrt(mean_square + EPSILON)
                normed_ref[r : r + GROUP, :] = (x32 * scale * gain_ref[...]).astype(jnp.bfloat16)

        @pl.when(i == 0)
        def _():
            key_copy.wait()
            value_copy.wait()

        both = jnp.dot(normed_ref[...], w_ref[...], preferred_element_type=jnp.float32)
        keys, values = both[:, :columns], both[:, columns:]
        heads = [
            jnp.where(low, keys, pltpu.roll(values, half, 1)).astype(jnp.bfloat16),
            jnp.where(low, pltpu.roll(keys, half, 1), values).astype(jnp.bfloat16),
        ]
        for h in range(2):
            head_ref[h, pl.ds(i * tile, tile), :] = heads[h]
            for j in range(tile_subs):
                place = places[h][j]
                for later in range(1, steps):
                    place = jnp.where(i == later, places[h][later * tile_subs + j], place)
                out_ref[place, 0 : rows // 2] = heads[h][j * rows : (j + 1) * rows].reshape(
                    rows // 2, 2, columns
                )
        return carry

    gain_copy.wait()
    lax.fori_loop(0, steps, multiply, 0)
    query_copy.wait()
    offset_copy.wait()

    low8 = lax.broadcasted_iota(jnp.int32, (8, columns), 1) < half
    query = jnp.broadcast_to(query_ref[...].astype(jnp.float32), (8, columns))
    queries = [
        jnp.where(low8, query, 0.0).astype(jnp.bfloat16),
        jnp.where(low8, pltpu.roll(query, half, 1), 0.0).astype(jnp.bfloat16),
    ]
    upper = (
        lax.broadcasted_iota(jnp.int32, (columns, columns), 0)
        > lax.broadcasted_iota(jnp.int32, (columns, columns), 1)
    ).astype(jnp.bfloat16)
    scores = jnp.concatenate(
        [
            lax.dot_general(
                queries[h], head_ref[h], (((1,), (1,)), ((), ())), preferred_element_type=jnp.float32
            )
            * half ** (-0.5)
            + offset_ref[h]
            for h in range(2)
        ],
        axis=0,
    )
    soft = jnp.log1p(jnp.exp(-jnp.abs(scores)))
    remain = -(jnp.maximum(scores, 0.0) + soft)
    taken = jnp.minimum(scores, 0.0) - soft
    pieces = [remain[:, c * columns : (c + 1) * columns] for c in range(chunks)]
    stacked = jnp.concatenate(
        [part.astype(jnp.bfloat16) for piece in pieces for part in split3(piece)], axis=0
    )
    summed = jnp.dot(stacked, upper, preferred_element_type=jnp.float32)
    later = jnp.zeros((16, 1), jnp.float32)
    after = [None] * chunks
    for c in reversed(range(chunks)):
        base = c * 48
        within = summed[base : base + 16] + summed[base + 16 : base + 32] + summed[base + 32 : base + 48]
        after[c] = within + later
        later = later + jnp.sum(pieces[c], axis=1, keepdims=True)
    sticks = jnp.exp(taken + jnp.concatenate(after, axis=1))
    rounded = sticks.astype(jnp.bfloat16).astype(jnp.float32)
    rest = sticks - rounded
    mixed = []
    for h in range(2):
        parts = jnp.concatenate([rounded[h * 8 : h * 8 + 8], rest[h * 8 : h * 8 + 8]], axis=0)
        products = jnp.dot(
            parts.astype(jnp.bfloat16), head_ref[h], preferred_element_type=jnp.float32
        )
        mixed.append(products[0:8] + products[8:16])

    line = lax.broadcasted_iota(jnp.int32, (8, columns), 0)
    lane = lax.broadcasted_iota(jnp.int32, (8, columns), 1)
    weighted = jnp.where(low8, pltpu.roll(mixed[0], half, 1), mixed[1])
    sums = jnp.zeros((8, columns), jnp.float32)
    for at, part in enumerate(split3(later[0:8]) + split3(later[8:16])):
        sums = jnp.where(lane == at, part, sums)
    payload = jnp.where(line == 0, weighted, sums)[0:2].astype(jnp.bfloat16)
    shape = (out_ref.shape[0], 1, 2, columns)
    out_ref[:, rows // 2 :] = jnp.broadcast_to(payload, shape)


def fill(rows, norm_gain, key_weight, value_weight, query, offset, order):
    count, width = rows.shape
    columns = key_weight.shape[1]
    heads = offset.shape[0]
    subs = len(order) // heads
    places = [[order.index(h * subs + j) for j in range(subs)] for h in range(heads)]
    tile = count // STEPS
    hbm = pl.BlockSpec(memory_space=pl.ANY)
    out_shape = (len(order), count // subs // 2 + 1, 2, columns)
    return pl.pallas_call(
        functools.partial(fill_kernel, places),
        in_specs=[hbm] * 6,
        out_specs=pl.BlockSpec(memory_space=pltpu.VMEM),
        out_shape=pltpu.VMEM(out_shape, jnp.bfloat16),
        scratch_shapes=[
            pltpu.VMEM((STEPS, tile, width), jnp.bfloat16),
            pltpu.VMEM((width, 2 * columns), jnp.bfloat16),
            pltpu.VMEM((1, width), jnp.float32),
            pltpu.VMEM((1, columns), jnp.bfloat16),
            pltpu.SMEM((heads,), jnp.float32),
            pltpu.VMEM((tile, width), jnp.bfloat16),
            pltpu.VMEM((heads, count, columns), jnp.bfloat16),
            pltpu.SemaphoreType.DMA((STEPS, PARTS)),
            pltpu.SemaphoreType.DMA((2,)),
            pltpu.SemaphoreType.DMA((3,)),
        ],
        name="fill",
    )(
        rows, norm_gain.reshape(1, width), key_weight, value_weight,
        query.reshape(1, columns), offset,
    )


def settle_kernel(
    order, moved_ref, gain_ref, keys_hbm, values_hbm, read_hbm, keys_ref, values_ref, read_ref, sem
):
    peers, rows, half = keys_ref.shape
    columns = 2 * half
    key_copy = pltpu.make_async_copy(keys_ref, keys_hbm, sem.at[0])
    value_copy = pltpu.make_async_copy(values_ref, values_hbm, sem.at[1])
    for at, block in enumerate(order):
        both = moved_ref[at, 0 : rows // 2].reshape(rows, columns)
        keys_ref[block] = both[:, :half]
        values_ref[block] = both[:, half:]
    key_copy.start()
    value_copy.start()

    payload = moved_ref[:, rows // 2].astype(jnp.float32)
    weighted, sums = payload[:, 0, :], payload[:, 1, :]
    at_row = lax.broadcasted_iota(jnp.int32, (peers, 1), 0)
    at_col = lax.broadcasted_iota(jnp.int32, (1, peers), 1)
    block_row, block_col = at_row, at_col
    for at, block in enumerate(order):
        block_row = jnp.where(at_row == at, block, block_row)
        block_col = jnp.where(at_col == at, block, block_col)
    after = jnp.where(block_col > block_row, 1.0, 0.0).astype(jnp.bfloat16)
    beyond = jnp.dot(after, sums.astype(jnp.bfloat16), preferred_element_type=jnp.float32)
    lane = lax.broadcasted_iota(jnp.int32, (peers, columns), 1)
    first = jnp.sum(jnp.where(lane < 3, beyond, 0.0), axis=1, keepdims=True)
    second = jnp.sum(jnp.where((lane >= 3) & (lane < 6), beyond, 0.0), axis=1, keepdims=True)
    low = lane < half
    mixed = jnp.sum(weighted * jnp.exp(jnp.where(low, first, second)), axis=0, keepdims=True)
    low = low[0:1]
    square = mixed * mixed
    first = jnp.sum(jnp.where(low, square, 0.0), axis=1, keepdims=True) / half
    second = jnp.sum(jnp.where(low, 0.0, square), axis=1, keepdims=True) / half
    scale = lax.rsqrt(jnp.where(low, first, second) + EPSILON)
    read_ref[...] = (mixed * scale * gain_ref[...]).astype(jnp.bfloat16)
    read_copy = pltpu.make_async_copy(read_ref, read_hbm, sem.at[2])
    read_copy.start()
    key_copy.wait()
    value_copy.wait()
    read_copy.wait()


def settle(moved, gain, order):
    peers, rows, _, columns = moved.shape
    rows, half = 2 * (rows - 1), columns // 2
    cache = jax.ShapeDtypeStruct((peers, rows, half), jnp.bfloat16)
    vmem = pl.BlockSpec(memory_space=pltpu.VMEM)
    hbm = pl.BlockSpec(memory_space=pl.ANY)
    buffer = pltpu.VMEM((peers, rows, half), jnp.bfloat16)
    return pl.pallas_call(
        functools.partial(settle_kernel, order),
        in_specs=[vmem, vmem],
        out_specs=[hbm, hbm, hbm],
        out_shape=[cache, cache, jax.ShapeDtypeStruct((1, columns), jnp.bfloat16)],
        scratch_shapes=[
            buffer, buffer, pltpu.VMEM((1, columns), jnp.bfloat16), pltpu.SemaphoreType.DMA((3,)),
        ],
        name="settle",
    )(
        pltpu.with_memory_space_constraint(moved, pltpu.VMEM),
        pltpu.with_memory_space_constraint(gain.reshape(1, columns), pltpu.VMEM),
    )


def body(prompt_rows, norm_gain, key_weight, value_weight, new_query, score_offset, output_gain):
    columns = key_weight.shape[1]
    peers = lax.axis_size("sp")
    order = ORDER if len(ORDER) == peers else list(range(peers))
    packed = fill(
        prompt_rows, norm_gain, key_weight, value_weight, new_query, score_offset, order
    )
    moved = lax.all_to_all(
        packed, "sp", split_axis=0, concat_axis=0, axis_index_groups=[order], tiled=True
    )
    keys, values, first_read = settle(moved, output_gain, order)
    target = (1, 1, *keys.shape)
    return (keys.reshape(target), values.reshape(target), first_read.reshape(columns))


def solution(mesh):
    in_specs = (
        P(("grp", "sp"), None),
        P(),
        P(None, "tp"),
        P(None, "tp"),
        P(("grp", "tp")),
        P("tp"),
        P("tp"),
    )
    out_specs = (
        P(("grp", "tp"), "sp", None, None, None),
        P(("grp", "tp"), "sp", None, None, None),
        P(("grp", "tp")),
    )
    return jax.shard_map(body, mesh=mesh, in_specs=in_specs, out_specs=out_specs, check_vma=False)
```

```python
import functools

import jax
import jax.numpy as jnp
from jax import lax
from jax.experimental import pallas as pl
from jax.experimental.pallas import tpu as pltpu
from jax.sharding import PartitionSpec as P

EPSILON = 1e-06
STEPS = 2
PARTS = 1
GROUP = 128
ORDER = [2 * (z + 4 * j) + c for c in (1, 0) for z in range(4) for j in range(4)]


def split3(value):
    high = value.astype(jnp.bfloat16).astype(jnp.float32)
    rest = value - high
    middle = rest.astype(jnp.bfloat16).astype(jnp.float32)
    return high, middle, rest - middle


def fill_kernel(
    places, x_hbm, gain_hbm, kw_hbm, vw_hbm, query_hbm, offset_hbm, out_ref,
    x_ref, w_ref, gain_ref, query_ref, offset_ref, normed_ref, head_ref, x_sem, w_sem, sem,
):
    steps, tile, _ = x_ref.shape
    columns = kw_hbm.shape[1]
    half = columns // 2
    rows = 2 * (out_ref.shape[1] - 1)
    count = steps * tile
    chunks = count // columns

    part = tile // PARTS

    def part_copy(i, p):
        return pltpu.make_async_copy(
            x_hbm.at[pl.ds(i * tile + p * part, part), :],
            x_ref.at[i, pl.ds(p * part, part), :],
            x_sem.at[i, p],
        )

    gain_copy = pltpu.make_async_copy(gain_hbm, gain_ref, sem.at[0])
    query_copy = pltpu.make_async_copy(query_hbm, query_ref, sem.at[1])
    offset_copy = pltpu.make_async_copy(offset_hbm, offset_ref, sem.at[2])
    key_copy = pltpu.make_async_copy(kw_hbm, w_ref.at[:, pl.ds(0, columns)], w_sem.at[0])
    value_copy = pltpu.make_async_copy(vw_hbm, w_ref.at[:, pl.ds(columns, columns)], w_sem.at[1])
    gain_copy.start()
    key_copy.start()
    value_copy.start()
    part_copy(0, 0).start()
    for i in range(steps):
        for p in range(PARTS):
            if i + p:
                part_copy(i, p).start(priority=1)
    query_copy.start(priority=1)
    offset_copy.start(priority=1)

    low = lax.broadcasted_iota(jnp.int32, (tile, columns), 1) < half

    tile_subs = tile // rows

    def multiply(i, carry):
        for p in range(PARTS):
            part_copy(i, p).wait()
            for r in range(p * part, (p + 1) * part, GROUP):
                x32 = x_ref[i, r : r + GROUP, :].astype(jnp.float32)
                mean_square = jnp.mean(x32 * x32, axis=-1, keepdims=True)
                scale = lax.rsqrt(mean_square + EPSILON)
                normed_ref[r : r + GROUP, :] = (x32 * scale * gain_ref[...]).astype(jnp.bfloat16)

        both = jnp.dot(normed_ref[...], w_ref[...], preferred_element_type=jnp.float32)
        keys, values = both[:, :columns], both[:, columns:]
        heads = [
            jnp.where(low, keys, pltpu.roll(values, half, 1)).astype(jnp.bfloat16),
            jnp.where(low, pltpu.roll(keys, half, 1), values).astype(jnp.bfloat16),
        ]
        for h in range(2):
            head_ref[h, pl.ds(i * tile, tile), :] = heads[h]
            for j in range(tile_subs):
                place = places[h][j]
                for later in range(1, steps):
                    place = jnp.where(i == later, places[h][later * tile_subs + j], place)
                out_ref[place, 0 : rows // 2] = heads[h][j * rows : (j + 1) * rows].reshape(
                    rows // 2, 2, columns
                )
        return carry

    gain_copy.wait()
    key_copy.wait()
    value_copy.wait()
    lax.fori_loop(0, steps, multiply, 0)
    query_copy.wait()
    offset_copy.wait()

    low8 = lax.broadcasted_iota(jnp.int32, (8, columns), 1) < half
    query = jnp.broadcast_to(query_ref[...].astype(jnp.float32), (8, columns))
    queries = [
        jnp.where(low8, query, 0.0).astype(jnp.bfloat16),
        jnp.where(low8, pltpu.roll(query, half, 1), 0.0).astype(jnp.bfloat16),
    ]
    upper = (
        lax.broadcasted_iota(jnp.int32, (columns, columns), 0)
        > lax.broadcasted_iota(jnp.int32, (columns, columns), 1)
    ).astype(jnp.bfloat16)
    scores = jnp.concatenate(
        [
            lax.dot_general(
                queries[h], head_ref[h], (((1,), (1,)), ((), ())), preferred_element_type=jnp.float32
            )
            * half ** (-0.5)
            + offset_ref[h]
            for h in range(2)
        ],
        axis=0,
    )
    soft = jnp.log1p(jnp.exp(-jnp.abs(scores)))
    remain = -(jnp.maximum(scores, 0.0) + soft)
    taken = jnp.minimum(scores, 0.0) - soft
    pieces = [remain[:, c * columns : (c + 1) * columns] for c in range(chunks)]
    stacked = jnp.concatenate(
        [part.astype(jnp.bfloat16) for piece in pieces for part in split3(piece)], axis=0
    )
    summed = jnp.dot(stacked, upper, preferred_element_type=jnp.float32)
    later = jnp.zeros((16, 1), jnp.float32)
    after = [None] * chunks
    for c in reversed(range(chunks)):
        base = c * 48
        within = summed[base : base + 16] + summed[base + 16 : base + 32] + summed[base + 32 : base + 48]
        after[c] = within + later
        later = later + jnp.sum(pieces[c], axis=1, keepdims=True)
    sticks = jnp.exp(taken + jnp.concatenate(after, axis=1))
    rounded = sticks.astype(jnp.bfloat16).astype(jnp.float32)
    rest = sticks - rounded
    mixed = []
    for h in range(2):
        parts = jnp.concatenate([rounded[h * 8 : h * 8 + 8], rest[h * 8 : h * 8 + 8]], axis=0)
        products = jnp.dot(
            parts.astype(jnp.bfloat16), head_ref[h], preferred_element_type=jnp.float32
        )
        mixed.append(products[0:8] + products[8:16])

    line = lax.broadcasted_iota(jnp.int32, (8, columns), 0)
    lane = lax.broadcasted_iota(jnp.int32, (8, columns), 1)
    weighted = jnp.where(low8, pltpu.roll(mixed[0], half, 1), mixed[1])
    sums = jnp.zeros((8, columns), jnp.float32)
    for at, part in enumerate(split3(later[0:8]) + split3(later[8:16])):
        sums = jnp.where(lane == at, part, sums)
    payload = jnp.where(line == 0, weighted, sums)[0:2].astype(jnp.bfloat16)
    shape = (out_ref.shape[0], 1, 2, columns)
    out_ref[:, rows // 2 :] = jnp.broadcast_to(payload, shape)


def fill(rows, norm_gain, key_weight, value_weight, query, offset, order):
    count, width = rows.shape
    columns = key_weight.shape[1]
    heads = offset.shape[0]
    subs = len(order) // heads
    places = [[order.index(h * subs + j) for j in range(subs)] for h in range(heads)]
    tile = count // STEPS
    hbm = pl.BlockSpec(memory_space=pl.ANY)
    out_shape = (len(order), count // subs // 2 + 1, 2, columns)
    return pl.pallas_call(
        functools.partial(fill_kernel, places),
        in_specs=[hbm] * 6,
        out_specs=pl.BlockSpec(memory_space=pltpu.VMEM),
        out_shape=pltpu.VMEM(out_shape, jnp.bfloat16),
        scratch_shapes=[
            pltpu.VMEM((STEPS, tile, width), jnp.bfloat16),
            pltpu.VMEM((width, 2 * columns), jnp.bfloat16),
            pltpu.VMEM((1, width), jnp.float32),
            pltpu.VMEM((1, columns), jnp.bfloat16),
            pltpu.SMEM((heads,), jnp.float32),
            pltpu.VMEM((tile, width), jnp.bfloat16),
            pltpu.VMEM((heads, count, columns), jnp.bfloat16),
            pltpu.SemaphoreType.DMA((STEPS, PARTS)),
            pltpu.SemaphoreType.DMA((2,)),
            pltpu.SemaphoreType.DMA((3,)),
        ],
        name="fill",
    )(
        rows, norm_gain.reshape(1, width), key_weight, value_weight,
        query.reshape(1, columns), offset,
    )


def settle_kernel(
    order, moved_ref, gain_ref, keys_hbm, values_hbm, read_hbm, keys_ref, values_ref, read_ref, sem
):
    peers, rows, half = keys_ref.shape
    columns = 2 * half
    key_copy = pltpu.make_async_copy(keys_ref, keys_hbm, sem.at[0])
    value_copy = pltpu.make_async_copy(values_ref, values_hbm, sem.at[1])
    for at, block in enumerate(order):
        both = moved_ref[at, 0 : rows // 2].reshape(rows, columns)
        keys_ref[block] = both[:, :half]
        values_ref[block] = both[:, half:]
    key_copy.start()
    value_copy.start()

    payload = moved_ref[:, rows // 2].astype(jnp.float32)
    weighted, sums = payload[:, 0, :], payload[:, 1, :]
    at_row = lax.broadcasted_iota(jnp.int32, (peers, 1), 0)
    at_col = lax.broadcasted_iota(jnp.int32, (1, peers), 1)
    block_row, block_col = at_row, at_col
    for at, block in enumerate(order):
        block_row = jnp.where(at_row == at, block, block_row)
        block_col = jnp.where(at_col == at, block, block_col)
    after = jnp.where(block_col > block_row, 1.0, 0.0).astype(jnp.bfloat16)
    beyond = jnp.dot(after, sums.astype(jnp.bfloat16), preferred_element_type=jnp.float32)
    lane = lax.broadcasted_iota(jnp.int32, (peers, columns), 1)
    first = jnp.sum(jnp.where(lane < 3, beyond, 0.0), axis=1, keepdims=True)
    second = jnp.sum(jnp.where((lane >= 3) & (lane < 6), beyond, 0.0), axis=1, keepdims=True)
    low = lane < half
    mixed = jnp.sum(weighted * jnp.exp(jnp.where(low, first, second)), axis=0, keepdims=True)
    low = low[0:1]
    square = mixed * mixed
    first = jnp.sum(jnp.where(low, square, 0.0), axis=1, keepdims=True) / half
    second = jnp.sum(jnp.where(low, 0.0, square), axis=1, keepdims=True) / half
    scale = lax.rsqrt(jnp.where(low, first, second) + EPSILON)
    read_ref[...] = (mixed * scale * gain_ref[...]).astype(jnp.bfloat16)
    read_copy = pltpu.make_async_copy(read_ref, read_hbm, sem.at[2])
    read_copy.start()
    key_copy.wait()
    value_copy.wait()
    read_copy.wait()


def settle(moved, gain, order):
    peers, rows, _, columns = moved.shape
    rows, half = 2 * (rows - 1), columns // 2
    cache = jax.ShapeDtypeStruct((peers, rows, half), jnp.bfloat16)
    vmem = pl.BlockSpec(memory_space=pltpu.VMEM)
    hbm = pl.BlockSpec(memory_space=pl.ANY)
    buffer = pltpu.VMEM((peers, rows, half), jnp.bfloat16)
    return pl.pallas_call(
        functools.partial(settle_kernel, order),
        in_specs=[vmem, vmem],
        out_specs=[hbm, hbm, hbm],
        out_shape=[cache, cache, jax.ShapeDtypeStruct((1, columns), jnp.bfloat16)],
        scratch_shapes=[
            buffer, buffer, pltpu.VMEM((1, columns), jnp.bfloat16), pltpu.SemaphoreType.DMA((3,)),
        ],
        name="settle",
    )(
        pltpu.with_memory_space_constraint(moved, pltpu.VMEM),
        pltpu.with_memory_space_constraint(gain.reshape(1, columns), pltpu.VMEM),
    )


def body(prompt_rows, norm_gain, key_weight, value_weight, new_query, score_offset, output_gain):
    columns = key_weight.shape[1]
    peers = lax.axis_size("sp")
    order = ORDER if len(ORDER) == peers else list(range(peers))
    packed = fill(
        prompt_rows, norm_gain, key_weight, value_weight, new_query, score_offset, order
    )
    moved = lax.all_to_all(
        packed, "sp", split_axis=0, concat_axis=0, axis_index_groups=[order], tiled=True
    )
    keys, values, first_read = settle(moved, output_gain, order)
    target = (1, 1, *keys.shape)
    return (keys.reshape(target), values.reshape(target), first_read.reshape(columns))


def solution(mesh):
    in_specs = (
        P(("grp", "sp"), None),
        P(),
        P(None, "tp"),
        P(None, "tp"),
        P(("grp", "tp")),
        P("tp"),
        P("tp"),
    )
    out_specs = (
        P(("grp", "tp"), "sp", None, None, None),
        P(("grp", "tp"), "sp", None, None, None),
        P(("grp", "tp")),
    )
    return jax.shard_map(body, mesh=mesh, in_specs=in_specs, out_specs=out_specs, check_vma=False)
```
